32 devices in a mesh: grp: 2 (over y), fs: 4 (over z), tp: 4 (over x, core).
Axes of the slice: x: 2, y: 2, z: 4, core: 2. Of those that a mesh axis runs over, the one named last changes fastest.
Arguments:
- layer_input_tokens: bfloat16 [4096, 2048], P(('grp', 'fs')), parts along dimension 0, may hold values from -6 to 6
- attention_norm_gain: float32 [2048], replicated, may hold values from 0.1 to 1.9
- query_projection: bfloat16 [2048, 1024], P('fs', 'tp'), may hold values from -0.125 to 0.125
- key_projection: bfloat16 [2048, 1024], P('fs', 'tp'), may hold values from -0.125 to 0.125
- value_projection: bfloat16 [2048, 2048], P('fs', 'tp'), may hold values from -0.125 to 0.125
- decay_first_factor: bfloat16 [2048, 16], replicated, may hold values from -0.125 to 0.125
- decay_second_factor: bfloat16 [16, 1024], P(None, 'tp'), may hold values from -1.5 to 1.5
- decay_logit_bias: float32 [1024], P('tp'), may hold values from -0.5 to 6
- extra_log_decay: float32 [4096, 8], P(('grp', 'fs'), 'tp'), parts along dimension 0, may hold values from -0.7 to 0
- head_output_gain: float32 [256], replicated, may hold values from 0.1 to 1.9
- attention_output_projection: bfloat16 [2048, 2048], P(('tp', 'fs')), may hold values from -0.125 to 0.125
- feedforward_norm_gain: float32 [2048], replicated, may hold values from 0.1 to 1.9
- gate_projection: bfloat16 [2048, 5632], P('fs', 'tp'), may hold values from -0.125 to 0.125
- up_projection: bfloat16 [2048, 5632], P('fs', 'tp'), may hold values from -0.125 to 0.125
- down_projection: bfloat16 [5632, 2048], P(('tp', 'fs')), may hold values from -0.078125 to 0.078125
Outputs:
- result: bfloat16 [4096, 2048], P(('grp', 'fs')), parts along dimension 0
The draws below stay inside these ranges and needn't reach their ends.
There are 2 independent parts, one for each index of `grp`. The reference program is written for one: setup_inputs(seed, part) draws one part's arguments, and reference() takes and returns one part's arrays. A program takes and returns all parts, laid end to end along the dimension named above; an argument that names none is the same for every part. Nothing has to cross between parts.
All inputs are finite; a program needn't handle non-finite values.
Results may differ from the reference program's by a relative error of at most 0.02.
Values may be sent and summed in bfloat16 or wider, within the bound.
A program may use at most 64 MiB of HBM per device.

```python
import jax
import jax.numpy as jnp
from jax import lax

D = 2048
HEADS = 8
KEY_CHANNELS = 128
DV = 256
RANK = 16
FF = 5632
BLOCK = 64
SEQ_LEN = 512
TOKENS = 2048
N_FS = 4
N_TP = 4


def draw_decay_logit_bias(key, part):
    pick = jax.random.randint(jax.random.fold_in(key, 11), (HEADS * KEY_CHANNELS,), 0, 10)
    fast = jax.random.uniform(jax.random.fold_in(key, 12), (HEADS * KEY_CHANNELS,), jnp.float32, -0.5, 1.0)
    slow = jax.random.uniform(jax.random.fold_in(key, 13), (HEADS * KEY_CHANNELS,), jnp.float32, 3.5, 5.5)
    return jnp.where(pick < 5, fast, slow).astype(jnp.float32)


def draw_extra_log_decay(key, part):
    hits = jax.random.randint(jax.random.fold_in(key, 21), (TOKENS, HEADS), 0, SEQ_LEN)
    depth = jnp.log(jax.random.uniform(jax.random.fold_in(key, 22), (TOKENS, HEADS), jnp.float32, 0.5, 0.8))
    return jnp.where(hits < 3, depth, 0.0).astype(jnp.float32)


def shard_levels(stream_key, extent, cuts, smallest, largest):
    def one(dim, parts):
        steps = jax.random.uniform(jax.random.fold_in(jax.random.fold_in(stream_key, 6), dim), (parts,), jnp.float32, smallest / len(cuts), largest / len(cuts))
        return jnp.repeat(jnp.exp(steps), extent[dim] // parts).reshape((-1,) + (1,) * (len(extent) - dim - 1))

    level = one(*cuts[0])
    for cut in cuts[1:]:
        level = level * one(*cut)
    return level


def noise(own_key, dims, deviation, most, cuts=(), held_as=jnp.bfloat16):
    entries = deviation * jax.random.normal(own_key, dims, jnp.float32)
    if cuts:
        entries = entries * shard_levels(own_key, dims, cuts, -0.22, 0.18)
    return jnp.clip(entries, -most, most).astype(held_as)


def setup_inputs(seed: int = 0, part: int = 0) -> dict:
    seeds = jax.random.split(jax.random.key(seed), 16)
    part_splits = jax.random.split(jax.random.fold_in(seeds[15], part), 16)
    layer_input_tokens = noise(part_splits[0], (TOKENS, D), 1.0, 6.0, ((0, 4),))
    attention_norm_gain = jnp.clip(1.0 + 0.18 * jax.random.normal(seeds[1], (D,), jnp.float32), 0.1, 1.9)
    query_projection = noise(seeds[2], (D, HEADS * KEY_CHANNELS), D ** -0.5, 0.125, ((0, 4), (1, 4)))
    key_projection = noise(seeds[3], (D, HEADS * KEY_CHANNELS), D ** -0.5, 0.125, ((0, 4), (1, 4)))
    value_projection = noise(seeds[4], (D, HEADS * DV), D ** -0.5, 0.125, ((0, 4), (1, 4)))
    decay_first_factor = noise(seeds[5], (D, RANK), D ** -0.5, 0.125)
    decay_second_factor = noise(seeds[6], (RANK, HEADS * KEY_CHANNELS), RANK ** -0.5, 1.5, ((1, 4),))
    decay_logit_bias = draw_decay_logit_bias(jax.random.fold_in(seeds[15], 71), part)
    extra_log_decay = draw_extra_log_decay(jax.random.fold_in(jax.random.fold_in(seeds[15], part), 71), part)
    head_output_gain = jnp.clip(1.0 + 0.18 * jax.random.normal(seeds[9], (DV,), jnp.float32), 0.1, 1.9)
    attention_output_projection = noise(seeds[10], (HEADS * DV, D), (HEADS * DV) ** -0.5, 0.125, ((0, 16),))
    feedforward_norm_gain = jnp.clip(1.0 + 0.18 * jax.random.normal(seeds[11], (D,), jnp.float32), 0.1, 1.9)
    gate_projection = noise(seeds[12], (D, FF), D ** -0.5, 0.125, ((0, 4), (1, 4)))
    up_projection = noise(seeds[13], (D, FF), D ** -0.5, 0.125, ((0, 4), (1, 4)))
    down_projection = noise(seeds[14], (FF, D), FF ** -0.5, 0.078125, ((0, 16),))
    return {"layer_input_tokens": layer_input_tokens, "attention_norm_gain": attention_norm_gain, "query_projection": query_projection, "key_projection": key_projection, "value_projection": value_projection, "decay_first_factor": decay_first_factor, "decay_second_factor": decay_second_factor, "decay_logit_bias": decay_logit_bias, "extra_log_decay": extra_log_decay, "head_output_gain": head_output_gain, "attention_output_projection": attention_output_projection, "feedforward_norm_gain": feedforward_norm_gain, "gate_projection": gate_projection, "up_projection": up_projection, "down_projection": down_projection}


normed_gate = 16.0

def norm_rows(values, gain):
    wide = values.astype(jnp.float32)
    scale = lax.rsqrt(lax.optimization_barrier(jnp.mean(wide * wide, axis=-1, keepdims=True)) + 1e-06)
    return wide * scale * gain

def block_scan(queries, keys, values, decays):
    length, key_channel_width = queries.shape
    value_width = values.shape[1]
    count = length // BLOCK
    lower_mask = jnp.arange(BLOCK)[:, None] >= jnp.arange(BLOCK)[None, :]

    def advance(carry, items):
        query_block, key_block, value_block, decay_block = items
        running = jnp.cumsum(decay_block, axis=0)
        middle = running[BLOCK // 2 - 1]
        closing = running[BLOCK - 1]
        carried = jnp.dot(query_block * jnp.exp(running), carry, precision=lax.Precision.HIGHEST)
        scores = jnp.dot(query_block * jnp.exp(running - middle), (key_block * jnp.exp(middle - running)).T, precision=lax.Precision.HIGHEST)
        scores = jnp.where(lower_mask, scores, 0.0)
        inside = jnp.dot(scores, value_block, precision=lax.Precision.HIGHEST)
        fresh = carry * jnp.exp(closing)[:, None] + jnp.dot((key_block * jnp.exp(closing - running)).T, value_block, precision=lax.Precision.HIGHEST)
        return (fresh, carried + inside)
    items = (queries.reshape(count, BLOCK, key_channel_width), keys.reshape(count, BLOCK, key_channel_width), values.reshape(count, BLOCK, value_width), decays.reshape(count, BLOCK, key_channel_width))
    _, outputs = lax.scan(advance, jnp.zeros((key_channel_width, value_width), jnp.float32), items)
    return outputs.reshape(length, value_width)

def both_ways(queries, keys, values, decays):
    ahead = block_scan(queries, keys, values, decays)
    behind = block_scan(jnp.flip(queries, 0), jnp.flip(keys, 0), jnp.flip(values, 0), jnp.flip(decays, 0))
    return ahead + jnp.flip(behind, 0)

def head_norm(mixed, gain):
    scale = lax.rsqrt(lax.optimization_barrier(jnp.mean(mixed * mixed, axis=-1, keepdims=True)) + 1e-06)
    return mixed * scale * gain

def group_sum(left, right):
    width = left.shape[1] // N_TP
    total = jnp.zeros((left.shape[0], right.shape[1]), jnp.float32)
    for group in range(N_TP):
        part = jnp.dot(left[:, group * width:(group + 1) * width], right[group * width:(group + 1) * width], preferred_element_type=jnp.float32)
        part = lax.optimization_barrier(part.astype(jnp.bfloat16))
        total = total + part.astype(jnp.float32)
    return total

def reference(layer_input_tokens, attention_norm_gain, query_projection, key_projection, value_projection, decay_first_factor, decay_second_factor, decay_logit_bias, extra_log_decay, head_output_gain, attention_output_projection, feedforward_norm_gain, gate_projection, up_projection, down_projection):
    normed = norm_rows(layer_input_tokens, attention_norm_gain).astype(jnp.bfloat16)
    query = jnp.dot(normed, query_projection, preferred_element_type=jnp.float32).astype(jnp.bfloat16)
    key = jnp.dot(normed, key_projection, preferred_element_type=jnp.float32).astype(jnp.bfloat16)
    value = jnp.dot(normed, value_projection, preferred_element_type=jnp.float32).astype(jnp.bfloat16)
    lowrank = jnp.dot(normed, decay_first_factor, preferred_element_type=jnp.float32).astype(jnp.bfloat16)
    decay_logit_values = jnp.dot(lowrank, decay_second_factor, preferred_element_type=jnp.float32) + decay_logit_bias
    decay_logarithm = jax.nn.log_sigmoid(decay_logit_values) / normed_gate + jnp.repeat(extra_log_decay, KEY_CHANNELS, axis=1)

    def sequences(array, width):
        return array.astype(jnp.float32).reshape(N_FS, SEQ_LEN, HEADS, width)
    mixed = jax.vmap(jax.vmap(both_ways, in_axes=1, out_axes=1))(sequences(query, KEY_CHANNELS), sequences(key, KEY_CHANNELS), sequences(value, DV), sequences(decay_logarithm, KEY_CHANNELS))
    headed = head_norm(mixed.reshape(TOKENS, HEADS, DV), head_output_gain)
    headed = headed.reshape(TOKENS, HEADS * DV).astype(jnp.bfloat16)
    mixer = group_sum(headed, attention_output_projection)
    residual = (layer_input_tokens.astype(jnp.float32) + mixer).astype(jnp.bfloat16)
    second = norm_rows(residual, feedforward_norm_gain).astype(jnp.bfloat16)
    gate = jnp.dot(second, gate_projection, preferred_element_type=jnp.float32)
    up = jnp.dot(second, up_projection, preferred_element_type=jnp.float32)
    hidden = (jax.nn.silu(gate) * up).astype(jnp.bfloat16)
    channel = group_sum(hidden, down_projection)
    return (residual.astype(jnp.float32) + channel).astype(jnp.bfloat16)
```

```python
import functools

import jax
import jax.numpy as jnp
from jax import lax
from jax.experimental import pallas as pl
from jax.experimental.pallas import tpu as pltpu
from jax.sharding import PartitionSpec as P

BLOCK = 64
DECAY_GATE = 16.0


def norm_rows(values, gain):
    wide = values.astype(jnp.float32)
    scale = lax.rsqrt(jnp.mean(wide * wide, axis=-1, keepdims=True) + 1e-06)
    return wide * scale * gain


def attention_kernel(heads, qkv_ref, lowrank_ref, second_ref, bias_ref, extra_ref, gain_ref, out_ref):
    rows = qkv_ref.shape[0]
    kc = second_ref.shape[1] // heads
    vc = out_ref.shape[1] // heads
    count = rows // BLOCK
    f32, bf16 = jnp.float32, jnp.bfloat16
    row_id = lax.broadcasted_iota(jnp.int32, (BLOCK, BLOCK), 0)
    col_id = lax.broadcasted_iota(jnp.int32, (BLOCK, BLOCK), 1)
    lower = row_id >= col_id
    upper = row_id <= col_id
    lower_ones = jnp.where(lower, 1.0, 0.0).astype(f32)
    half = BLOCK // 2
    for h in range(heads):
        kcols = slice(h * kc, (h + 1) * kc)
        logits = (
            jnp.dot(lowrank_ref[...], second_ref[:, kcols], preferred_element_type=f32)
            + bias_ref[:, kcols]
        )
        log_sig = jnp.minimum(logits, 0.0) - jnp.log1p(jnp.exp(-jnp.abs(logits)))
        decay = log_sig / DECAY_GATE + extra_ref[:, h : h + 1]
        queries_fb, updates, closings, scores = [], [], [], []
        for b in range(count):
            r = slice(b * BLOCK, (b + 1) * BLOCK)
            d = decay[r]
            q = qkv_ref[r, h * kc : (h + 1) * kc].astype(f32)
            k = qkv_ref[r, (heads + h) * kc : (heads + h + 1) * kc].astype(f32)
            v = qkv_ref[r, 2 * heads * kc + h * vc : 2 * heads * kc + (h + 1) * vc]
            run = jnp.dot(lower_ones, d, precision=lax.Precision.HIGHEST, preferred_element_type=f32)
            closing = run[BLOCK - 1 : BLOCK]
            back = closing - run + d
            mid_f = run[half - 1 : half]
            mid_b = back[half : half + 1]
            qf = (q * jnp.exp(run - mid_f)).astype(bf16)
            kf = (k * jnp.exp(mid_f - run)).astype(bf16)
            qb = (q * jnp.exp(back - mid_b)).astype(bf16)
            kb = (k * jnp.exp(mid_b - back)).astype(bf16)
            nt = (((1,), (1,)), ((), ()))
            sf = lax.dot_general(qf, kf, nt, preferred_element_type=f32)
            sb = lax.dot_general(qb, kb, nt, preferred_element_type=f32)
            scores.append(
                (jnp.where(lower, sf, 0.0) + jnp.where(upper, sb, 0.0)).astype(bf16)
            )
            queries_fb.append(
                jnp.concatenate([q * jnp.exp(run), q * jnp.exp(back)], axis=1).astype(bf16)
            )
            keys_fb = jnp.concatenate(
                [k * jnp.exp(closing - run), k * jnp.exp(closing - back)], axis=1
            ).astype(bf16)
            updates.append(
                lax.dot_general(v, keys_fb, (((0,), (0,)), ((), ())), preferred_element_type=f32)
            )
            closings.append(jnp.exp(closing))
        state = jnp.zeros((vc, kc), f32)
        ahead = []
        for b in range(count):
            ahead.append(state.astype(bf16))
            state = state * closings[b] + updates[b][:, :kc]
        state = jnp.zeros((vc, kc), f32)
        behind = [None] * count
        for b in reversed(range(count)):
            behind[b] = state.astype(bf16)
            state = state * closings[b] + updates[b][:, kc:]
        for b in range(count):
            r = slice(b * BLOCK, (b + 1) * BLOCK)
            v = qkv_ref[r, 2 * heads * kc + h * vc : 2 * heads * kc + (h + 1) * vc]
            states = jnp.concatenate([ahead[b], behind[b]], axis=1)
            mixed = lax.dot_general(
                queries_fb[b], states, (((1,), (1,)), ((), ())), preferred_element_type=f32
            ) + jnp.dot(scores[b], v, preferred_element_type=f32)
            scale = lax.rsqrt(jnp.mean(mixed * mixed, axis=-1, keepdims=True) + 1e-06)
            out_ref[r, h * vc : (h + 1) * vc] = (mixed * scale * gain_ref[...]).astype(bf16)


def attention(qkv, lowrank, second_factor, bias, extra, gain):
    rows = qkv.shape[0]
    heads = extra.shape[1]
    width = heads * gain.shape[0]
    kc = second_factor.shape[1] // heads
    return pl.pallas_call(
        functools.partial(attention_kernel, heads),
        out_shape=jax.ShapeDtypeStruct((rows, width), jnp.bfloat16),
        in_specs=[pl.BlockSpec(memory_space=pltpu.VMEM)] * 6,
        out_specs=pl.BlockSpec(memory_space=pltpu.VMEM),
        compiler_params=pltpu.CompilerParams(vmem_limit_bytes=32 * 1024 * 1024),
        cost_estimate=pl.CostEstimate(
            flops=40 * rows * kc * width, bytes_accessed=4 * rows * width * 2, transcendentals=0
        ),
    )(qkv, lowrank, second_factor, bias[None, :], extra, gain[None, :])


def gather_shared(piece):
    copies = lax.axis_size("grp")
    depth = piece.shape[0]
    if depth % copies:
        return lax.all_gather(piece, "fs", axis=0, tiled=True)
    part = depth // copies
    own = lax.dynamic_slice_in_dim(piece, lax.axis_index("grp") * part, part, 0)
    return lax.all_gather(own, ("fs", "grp"), axis=0, tiled=True)


def step_back(values, hops):
    count = lax.axis_size("tp")
    return lax.ppermute(values, "tp", [(i, (i - hops) % count) for i in range(count)])


def step_on(values, hops):
    count = lax.axis_size("tp")
    return lax.ppermute(values, "tp", [(i, (i + hops) % count) for i in range(count)])


def scatter_sum(partial, share):
    count = lax.axis_size("tp")
    total = partial[:share].astype(jnp.float32)
    arrived = [step_back(partial[j * share : (j + 1) * share], j) for j in range(1, count)]
    for block in arrived:
        total = total + block.astype(jnp.float32)
    return total


def shards(
    layer_input_tokens,
    attention_norm_gain,
    query_projection,
    key_projection,
    value_projection,
    decay_first_factor,
    decay_second_factor,
    decay_logit_bias,
    extra_log_decay,
    head_output_gain,
    attention_output_projection,
    feedforward_norm_gain,
    gate_projection,
    up_projection,
    down_projection,
):
    rows = layer_input_tokens.shape[0]
    count = lax.axis_size("tp")
    me = lax.axis_index("tp")
    share = rows // count
    qkv_full = gather_shared(
        jnp.concatenate([query_projection, key_projection, value_projection], axis=1)
    )
    out_full = gather_shared(attention_output_projection)
    gate_full = gather_shared(gate_projection)
    up_full = gather_shared(up_projection)
    down_full = gather_shared(down_projection)

    normed = norm_rows(layer_input_tokens, attention_norm_gain).astype(jnp.bfloat16)
    lowrank = jnp.dot(normed, decay_first_factor, preferred_element_type=jnp.float32).astype(
        jnp.bfloat16
    )
    qkv = jnp.dot(normed, qkv_full, preferred_element_type=jnp.float32).astype(jnp.bfloat16)
    headed = attention(
        qkv, lowrank, decay_second_factor, decay_logit_bias, extra_log_decay, head_output_gain
    )
    turned = jnp.concatenate(
        [
            lax.dynamic_slice_in_dim(headed, lax.rem(me - j + count, count) * share, share, 0)
            for j in range(count)
        ],
        axis=0,
    )
    mixer = scatter_sum(
        jnp.dot(turned, out_full, preferred_element_type=jnp.float32).astype(jnp.bfloat16), share
    )
    own = lax.dynamic_slice_in_dim(layer_input_tokens, me * share, share, 0)
    residual = (own.astype(jnp.float32) + mixer).astype(jnp.bfloat16)
    mine = norm_rows(residual, feedforward_norm_gain).astype(jnp.bfloat16)
    second = jnp.concatenate([mine] + [step_on(mine, j) for j in range(1, count)], axis=0)
    gate = jnp.dot(second, gate_full, preferred_element_type=jnp.float32)
    up = jnp.dot(second, up_full, preferred_element_type=jnp.float32)
    hidden = (jax.nn.silu(gate) * up).astype(jnp.bfloat16)
    channel = scatter_sum(
        jnp.dot(hidden, down_full, preferred_element_type=jnp.float32).astype(jnp.bfloat16), share
    )
    finished = (residual.astype(jnp.float32) + channel).astype(jnp.bfloat16)
    return lax.all_gather(finished, "tp", axis=0, tiled=True)


def solution(mesh):
    placed = (
        P(("grp", "fs"), None),
        P(),
        P("fs", "tp"),
        P("fs", "tp"),
        P("fs", "tp"),
        P(),
        P(None, "tp"),
        P("tp"),
        P(("grp", "fs"), "tp"),
        P(),
        P(("tp", "fs"), None),
        P(),
        P("fs", "tp"),
        P("fs", "tp"),
        P(("tp", "fs"), None),
    )
    return jax.shard_map(
        shards, mesh=mesh, in_specs=placed, out_specs=P(("grp", "fs"), None), check_vma=False
    )
```

```python
import functools

import jax
import jax.numpy as jnp
from jax import lax
from jax.experimental import pallas as pl
from jax.experimental.pallas import tpu as pltpu
from jax.sharding import PartitionSpec as P

BLOCK = 64
DECAY_GATE = 16.0


def norm_rows(values, gain):
    wide = values.astype(jnp.float32)
    scale = lax.rsqrt(jnp.mean(wide * wide, axis=-1, keepdims=True) + 1e-06)
    return wide * scale * gain


def attention_kernel(heads, qkv_ref, lowrank_ref, second_ref, bias_ref, extra_ref, gain_ref, out_ref):
    rows = qkv_ref.shape[0]
    kc = second_ref.shape[1] // heads
    vc = out_ref.shape[1] // heads
    count = rows // BLOCK
    f32, bf16 = jnp.float32, jnp.bfloat16
    row_id = lax.broadcasted_iota(jnp.int32, (BLOCK, BLOCK), 0)
    col_id = lax.broadcasted_iota(jnp.int32, (BLOCK, BLOCK), 1)
    lower = row_id >= col_id
    upper = row_id <= col_id
    lower_ones = jnp.where(lower, 1.0, 0.0).astype(f32)
    half = BLOCK // 2
    for h in range(heads):
        kcols = slice(h * kc, (h + 1) * kc)
        logits = (
            jnp.dot(lowrank_ref[...], second_ref[:, kcols], preferred_element_type=f32)
            + bias_ref[:, kcols]
        )
        log_sig = jnp.minimum(logits, 0.0) - jnp.log1p(jnp.exp(-jnp.abs(logits)))
        decay = log_sig / DECAY_GATE + extra_ref[:, h : h + 1]
        queries_fb, updates, closings, scores = [], [], [], []
        for b in range(count):
            r = slice(b * BLOCK, (b + 1) * BLOCK)
            d = decay[r]
            q = qkv_ref[r, h * kc : (h + 1) * kc].astype(f32)
            k = qkv_ref[r, (heads + h) * kc : (heads + h + 1) * kc].astype(f32)
            v = qkv_ref[r, 2 * heads * kc + h * vc : 2 * heads * kc + (h + 1) * vc]
            run = jnp.dot(lower_ones, d, precision=lax.Precision.HIGHEST, preferred_element_type=f32)
            closing = run[BLOCK - 1 : BLOCK]
            back = closing - run + d
            mid_f = run[half - 1 : half]
            mid_b = back[half : half + 1]
            qf = (q * jnp.exp(run - mid_f)).astype(bf16)
            kf = (k * jnp.exp(mid_f - run)).astype(bf16)
            qb = (q * jnp.exp(back - mid_b)).astype(bf16)
            kb = (k * jnp.exp(mid_b - back)).astype(bf16)
            nt = (((1,), (1,)), ((), ()))
            sf = lax.dot_general(qf, kf, nt, preferred_element_type=f32)
            sb = lax.dot_general(qb, kb, nt, preferred_element_type=f32)
            scores.append(
                (jnp.where(lower, sf, 0.0) + jnp.where(upper, sb, 0.0)).astype(bf16)
            )
            queries_fb.append(
                jnp.concatenate([q * jnp.exp(run), q * jnp.exp(back)], axis=1).astype(bf16)
            )
            keys_fb = jnp.concatenate(
                [k * jnp.exp(closing - run), k * jnp.exp(closing - back)], axis=1
            ).astype(bf16)
            updates.append(
                lax.dot_general(v, keys_fb, (((0,), (0,)), ((), ())), preferred_element_type=f32)
            )
            closings.append(jnp.exp(closing))
        state = jnp.zeros((vc, kc), f32)
        ahead = []
        for b in range(count):
            ahead.append(state.astype(bf16))
            state = state * closings[b] + updates[b][:, :kc]
        state = jnp.zeros((vc, kc), f32)
        behind = [None] * count
        for b in reversed(range(count)):
            behind[b] = state.astype(bf16)
            state = state * closings[b] + updates[b][:, kc:]
        for b in range(count):
            r = slice(b * BLOCK, (b + 1) * BLOCK)
            v = qkv_ref[r, 2 * heads * kc + h * vc : 2 * heads * kc + (h + 1) * vc]
            states = jnp.concatenate([ahead[b], behind[b]], axis=1)
            mixed = lax.dot_general(
                queries_fb[b], states, (((1,), (1,)), ((), ())), preferred_element_type=f32
            ) + jnp.dot(scores[b], v, preferred_element_type=f32)
            scale = lax.rsqrt(jnp.mean(mixed * mixed, axis=-1, keepdims=True) + 1e-06)
            out_ref[r, h * vc : (h + 1) * vc] = (mixed * scale * gain_ref[...]).astype(bf16)


def attention(qkv, lowrank, second_factor, bias, extra, gain):
    rows = qkv.shape[0]
    heads = extra.shape[1]
    width = heads * gain.shape[0]
    kc = second_factor.shape[1] // heads
    return pl.pallas_call(
        functools.partial(attention_kernel, heads),
        out_shape=jax.ShapeDtypeStruct((rows, width), jnp.bfloat16),
        in_specs=[pl.BlockSpec(memory_space=pltpu.VMEM)] * 6,
        out_specs=pl.BlockSpec(memory_space=pltpu.VMEM),
        compiler_params=pltpu.CompilerParams(vmem_limit_bytes=32 * 1024 * 1024),
        cost_estimate=pl.CostEstimate(
            flops=40 * rows * kc * width, bytes_accessed=4 * rows * width * 2, transcendentals=0
        ),
    )(qkv, lowrank, second_factor, bias[None, :], extra, gain[None, :])


def gather_shared(piece, chunks=1):
    copies = lax.axis_size("grp")
    if copies != 2 or piece.shape[1] % (copies * chunks):
        return [(lax.all_gather(piece, "fs", axis=0, tiled=True), None)]
    wide = piece.shape[1] // chunks
    part = wide // copies
    pairs = []
    for chunk in range(chunks):
        start = chunk * wide + lax.axis_index("grp") * part
        own = lax.all_gather(
            lax.dynamic_slice_in_dim(piece, start, part, 1), "fs", axis=0, tiled=True
        )
        pairs.append((own, lax.ppermute(own, "grp", [(0, 1), (1, 0)])))
    return pairs


def in_order(pairs):
    if pairs[0][1] is None:
        return pairs[0][0]
    first = lax.axis_index("grp") == 0
    blocks = []
    for own, other in pairs:
        blocks += [jnp.where(first, own, other), jnp.where(first, other, own)]
    return jnp.concatenate(blocks, axis=1)


def times(left, right):
    if right is None:
        return None
    return jnp.dot(left, right, preferred_element_type=jnp.float32)


def shared_dot(left, pairs):
    def rounded(right):
        return None if right is None else times(left, right).astype(jnp.bfloat16)

    return in_order([(rounded(own), rounded(other)) for own, other in pairs])


def gated(second, gate_weight, up_weight):
    if gate_weight is None:
        return None
    gate, up = times(second, gate_weight), times(second, up_weight)
    return (jax.nn.silu(gate) * up).astype(jnp.bfloat16)


def step_back(values, hops):
    count = lax.axis_size("tp")
    return lax.ppermute(values, "tp", [(i, (i - hops) % count) for i in range(count)])


def step_on(values, hops):
    count = lax.axis_size("tp")
    return lax.ppermute(values, "tp", [(i, (i + hops) % count) for i in range(count)])


def scatter_sum(partial, share):
    count = lax.axis_size("tp")
    total = partial[:share].astype(jnp.float32)
    arrived = [step_back(partial[j * share : (j + 1) * share], j) for j in range(1, count)]
    for block in arrived:
        total = total + block.astype(jnp.float32)
    return total


def shards(
    layer_input_tokens,
    attention_norm_gain,
    query_projection,
    key_projection,
    value_projection,
    decay_first_factor,
    decay_second_factor,
    decay_logit_bias,
    extra_log_decay,
    head_output_gain,
    attention_output_projection,
    feedforward_norm_gain,
    gate_projection,
    up_projection,
    down_projection,
):
    rows = layer_input_tokens.shape[0]
    count = lax.axis_size("tp")
    me = lax.axis_index("tp")
    share = rows // count
    qkv_full = gather_shared(
        jnp.concatenate([query_projection, key_projection, value_projection], axis=1)
    )
    out_full = gather_shared(attention_output_projection)
    gate_full = gather_shared(gate_projection)
    up_full = gather_shared(up_projection)
    down_full = gather_shared(down_projection, 2)

    normed = norm_rows(layer_input_tokens, attention_norm_gain).astype(jnp.bfloat16)
    lowrank = jnp.dot(normed, decay_first_factor, preferred_element_type=jnp.float32).astype(
        jnp.bfloat16
    )
    qkv = shared_dot(normed, qkv_full)
    headed = attention(
        qkv, lowrank, decay_second_factor, decay_logit_bias, extra_log_decay, head_output_gain
    )
    turned = jnp.concatenate(
        [
            lax.dynamic_slice_in_dim(headed, lax.rem(me - j + count, count) * share, share, 0)
            for j in range(count)
        ],
        axis=0,
    )
    mixer = scatter_sum(shared_dot(turned, out_full), share)
    own = lax.dynamic_slice_in_dim(layer_input_tokens, me * share, share, 0)
    residual = (own.astype(jnp.float32) + mixer).astype(jnp.bfloat16)
    mine = norm_rows(residual, feedforward_norm_gain).astype(jnp.bfloat16)
    second = jnp.concatenate([mine] + [step_on(mine, j) for j in range(1, count)], axis=0)
    hidden = in_order(
        [
            (gated(second, g_own, u_own), gated(second, g_other, u_other))
            for (g_own, g_other), (u_own, u_other) in zip(gate_full, up_full)
        ]
    )
    channel = scatter_sum(shared_dot(hidden, down_full), share)
    finished = (residual.astype(jnp.float32) + channel).astype(jnp.bfloat16)
    return lax.all_gather(finished, "tp", axis=0, tiled=True)


def solution(mesh):
    placed = (
        P(("grp", "fs"), None),
        P(),
        P("fs", "tp"),
        P("fs", "tp"),
        P("fs", "tp"),
        P(),
        P(None, "tp"),
        P("tp"),
        P(("grp", "fs"), "tp"),
        P(),
        P(("tp", "fs"), None),
        P(),
        P("fs", "tp"),
        P("fs", "tp"),
        P(("tp", "fs"), None),
    )
    return jax.shard_map(
        shards, mesh=mesh, in_specs=placed, out_specs=P(("grp", "fs"), None), check_vma=False
    )
```
